512 devices in a mesh: grp: 2 (over y), sp: 16 (over z), dp: 16 (over x, core).
Axes of the slice: x: 8, y: 2, z: 16, core: 2. Of those that a mesh axis runs over, the one named last changes fastest.
The devices are a block of a 8x8x16 slice.
Arguments:
- tokens: bfloat16 [32, 2560, 2048], P(('grp', 'dp'), 'sp'), parts along dimension 0, may hold values from -6 to 6
- query_weight: bfloat16 [2048, 1024], P('dp'), may hold values from -0.125 to 0.125
- key_weight: bfloat16 [2048, 256], P('dp'), may hold values from -0.125 to 0.125
- value_weight: bfloat16 [2048, 256], P('dp'), may hold values from -0.125 to 0.125
- out_weight: bfloat16 [1024, 2048], P(None, 'dp'), may hold values from -0.1875 to 0.1875
- query_gain: float32 [64], replicated, may hold values from 0.28 to 6
- key_gain: float32 [64], replicated, may hold values from 0.28 to 6
Outputs:
- mixed: bfloat16 [32, 2560, 2048], P(('grp', 'dp'), 'sp'), parts along dimension 0
The draws below stay inside these ranges and needn't reach their ends.
There are 2 independent parts, one for each index of `grp`. The reference program is written for one: setup_inputs(seed, part) draws one part's arguments, and reference() takes and returns one part's arrays. A program takes and returns all parts, laid end to end along the dimension named above; an argument that names none is the same for every part. Nothing has to cross between parts.
All inputs are finite; a program needn't handle non-finite values.
Results may differ from the reference program's by a relative error of at most 0.006.
The reference program's roundings to bfloat16 on the way count: a program that leaves them out, or rounds other values in their place, can miss the bound.
Values may be sent and summed in bfloat16 or wider, within the bound.
A program may use at most 64 MiB of HBM per device.

```python
import jax
import jax.numpy as jnp
from jax import lax

D = 2048
HEADS = 16
KV_HEADS = 4
HEAD_DIM = 64
GRID_W = 64
SEQ_LEN = 2560
SEQS = 16


def gain_values(key):
    return 1.0 + 0.18 * jnp.clip(jax.random.normal(key, (HEAD_DIM,), jnp.float32), -4.0, 4.0)


def draw_query_gain(key, part):
    return gain_values(jax.random.fold_in(key, 11))


def draw_key_gain(key, part):
    return gain_values(jax.random.fold_in(key, 23))


def level_of(rng, dims, split, least, largest):
    factor_of, own = 1.0, jax.random.fold_in(rng, 6)
    for position, blocks in split:
        steps = jnp.exp(jax.random.uniform(jax.random.fold_in(own, position), (blocks,), jnp.float32, least / len(split), largest / len(split)))
        factor_of = factor_of * jnp.repeat(steps, dims[position] // blocks).reshape([-1 if axis == position else 1 for axis in range(len(dims))])
    return factor_of


def gaussian(rng, shape, spread, bound, pieces=(), kind=jnp.bfloat16):
    values = jax.random.normal(rng, shape, jnp.float32) * spread
    if len(pieces) > 0:
        values = level_of(rng, shape, pieces, -0.22, 0.18) * values
    return jnp.clip(values, min=-bound, max=bound).astype(kind)


def setup_inputs(seed: int = 0, part: int = 0) -> dict:
    splits = jax.random.split(jax.random.key(seed), 8)
    part_splits = jax.random.split(jax.random.fold_in(splits[7], part), 8)
    tokens = gaussian(part_splits[0], (SEQS, SEQ_LEN, D), 1.0, 6.0, ((0, 16), (1, 16)))
    query_weight = gaussian(splits[1], (D, HEADS * HEAD_DIM), D ** -0.5, 0.125, ((0, 16),))
    key_weight = gaussian(splits[2], (D, KV_HEADS * HEAD_DIM), D ** -0.5, 0.125, ((0, 16),))
    value_weight = gaussian(splits[3], (D, KV_HEADS * HEAD_DIM), D ** -0.5, 0.125, ((0, 16),))
    out_weight = gaussian(splits[4], (HEADS * HEAD_DIM, D), (HEADS * HEAD_DIM) ** -0.5, 0.1875, ((1, 16),))
    query_gain = draw_query_gain(jax.random.fold_in(splits[7], 71), part)
    key_gain = draw_key_gain(jax.random.fold_in(splits[7], 71), part)
    return dict(tokens=tokens, query_weight=query_weight, key_weight=key_weight, value_weight=value_weight, out_weight=out_weight, query_gain=query_gain, key_gain=key_gain)


theta_base = 10000.0
norm_eps = 1e-06

def rotary_tables(positions):
    quarter = HEAD_DIM // 4
    inverse = theta_base ** (-jnp.arange(quarter, dtype=jnp.float32) / quarter)
    grid_rows = (positions // GRID_W).astype(jnp.float32)
    grid_cols = (positions % GRID_W).astype(jnp.float32)
    angles = jnp.concatenate([grid_rows[:, None] * inverse, grid_cols[:, None] * inverse], axis=-1)
    return (jnp.cos(angles), jnp.sin(angles))

def norm_rotate(raw, gain, cosine, sine):
    scaled = raw * lax.rsqrt(lax.optimization_barrier(jnp.mean(raw * raw, axis=-1, keepdims=True)) + norm_eps) * gain
    half = HEAD_DIM // 2
    first_half = scaled[..., :half]
    second_half = scaled[..., half:]
    cosine = cosine[:, None, :]
    sine = sine[:, None, :]
    turned = jnp.concatenate([first_half * cosine - second_half * sine, second_half * cosine + first_half * sine], axis=-1)
    return turned.astype(jnp.bfloat16)

def reference(tokens, query_weight, key_weight, value_weight, out_weight, query_gain, key_gain):
    length = tokens.shape[1]
    per_kv = HEADS // KV_HEADS
    cosine, sine = rotary_tables(jnp.arange(length, dtype=jnp.int32))
    scale = HEAD_DIM ** (-0.5)

    def one_sequence(rows_in):
        raw_q = jnp.dot(rows_in, query_weight, preferred_element_type=jnp.float32).reshape(length, HEADS, HEAD_DIM)
        raw_k = jnp.dot(rows_in, key_weight, preferred_element_type=jnp.float32).reshape(length, KV_HEADS, HEAD_DIM)
        values = jnp.dot(rows_in, value_weight, preferred_element_type=jnp.float32).astype(jnp.bfloat16)
        queries = norm_rotate(raw_q, query_gain, cosine, sine)
        keys = norm_rotate(raw_k, key_gain, cosine, sine)
        query_heads = queries.reshape(length, KV_HEADS, per_kv, HEAD_DIM).transpose(1, 0, 2, 3)
        key_heads = keys.transpose(1, 0, 2)
        value_heads = values.reshape(length, KV_HEADS, HEAD_DIM).transpose(1, 0, 2)

        def one_head(operands):
            head_q, head_k, head_v = operands
            scores = jnp.einsum('qgd,sd->gqs', head_q.astype(jnp.float32), head_k.astype(jnp.float32)) * scale
            top = lax.optimization_barrier(jnp.max(scores, axis=-1, keepdims=True))
            weights = jnp.exp(scores - top)
            probs = (weights / lax.optimization_barrier(jnp.sum(weights, axis=-1, keepdims=True))).astype(jnp.bfloat16)
            return jnp.einsum('gqs,sd->qgd', probs.astype(jnp.float32), head_v.astype(jnp.float32)).astype(jnp.bfloat16)
        attended = lax.map(one_head, (query_heads, key_heads, value_heads))
        attended = attended.transpose(1, 0, 2, 3).reshape(length, HEADS * HEAD_DIM)
        return jnp.dot(attended, out_weight, preferred_element_type=jnp.float32).astype(jnp.bfloat16)
    return lax.map(one_sequence, tokens)
```

```python
import math

import jax
import jax.numpy as jnp
from jax import lax
from jax.experimental import pallas as pl
from jax.experimental.pallas import tpu as pltpu
from jax.sharding import PartitionSpec as P

HEADS = 16
KV_HEADS = 4
HEAD_DIM = 64
GRID_W = 64
PER_KV = HEADS // KV_HEADS
HALF = HEAD_DIM // 2
QUARTER = HEAD_DIM // 4

theta_base = 10000.0
norm_eps = 1e-06
MESH = pl.DeviceIdType.MESH
ONES = 16
VROWS = HEAD_DIM + ONES

X_KV0, X_KV_STEP = 3.0, 2.9
X_W_STEP = 5.7
Z0, Z_STEP = 15.0, 3.55
UNIT_US = 1.3


def norm_rotate_t(raw, gain, cosine, sine):
    inv = lax.rsqrt(jnp.mean(raw * raw, axis=0, keepdims=True) + norm_eps)
    scaled = raw * inv * gain
    first, second = scaled[:HALF], scaled[HALF:]
    return jnp.concatenate(
        [first * cosine - second * sine, second * cosine + first * sine], axis=0
    )


def make_schedule(nx, nz):
    h, hz = nx // 2, nz // 2
    events = []
    t = X_KV0
    for cls in range(3):
        step = X_KV_STEP if cls == 0 else X_W_STEP
        for s in range(1, h + 1):
            for p in range(2):
                for d in range(2):
                    if s == h and p != d:
                        continue
                    at = t + (s - 1) * step + step * (0.5 + 0.5 * p if s < h else 0.5)
                    events.append((at, "w", cls, d, s, p))
        t += (h - 0.5) * step
    for s in range(1, hz + 1):
        for p in range(2):
            for d in range(2):
                if s == hz and p != d:
                    continue
                at = Z0 + (s - 1) * Z_STEP + Z_STEP * (0.5 + 0.5 * p if s < hz else 0.5) + 0.5
                events.append((at, "z", d, s, p))
    return sorted(events, key=lambda e: e[0])


def kernel(nx, nz, tok_in, wq_in, wk_in, wv_in, wo_in, qg_in, kg_in, out_ref,
           tok, wq, wk, wv, wo, kbuf, vbuf, vt, qbd, rawq, tab, acc, top, att,
           ring_recv, ring_send, d2d_recv, d2d_send, z_recv, z_send, loc):
    h_x, h_z = nx // 2, nz // 2
    rows = tok.shape[0]
    cols = PER_KV * rows
    dp = lax.axis_index("dp")
    z = lax.axis_index("sp")
    x, c = dp // 2, lax.rem(dp, 2)
    other = 1 - c
    to_x = ({"dp": lax.rem(dp + 2, 2 * nx)}, {"dp": lax.rem(dp + 2 * nx - 2, 2 * nx)})
    to_z = ({"sp": lax.rem(z + 1, nz)}, {"sp": lax.rem(z + nz - 1, nz)})
    to_core = {"dp": 2 * x + other}

    wrows = wk.shape[2]
    loads = []

    def load(src, dst):
        cp = pltpu.make_async_copy(src, dst, loc.at[len(loads)])
        cp.start()
        loads.append(cp)

    load(wk_in, wk.at[x, c])
    load(wv_in, wv.at[x, c])
    load(tok_in.at[0], tok)
    for p in range(2):
        load(wq_in.at[pl.ds(p * (wrows // 2), wrows // 2)], wq.at[x, c, p])
    orows = wo.shape[3]
    for p in range(2):
        load(wo_in.at[pl.ds(p * orows, orows)], wo.at[x, c, p])

    barrier = pltpu.get_barrier_semaphore()
    for peer in (*to_x, *to_z, to_core):
        pl.semaphore_signal(barrier, inc=1, device_id=peer, device_id_type=MESH)

    t = lax.broadcasted_iota(jnp.int32, (HALF, cols), 1)
    for _ in range(PER_KV - 1):
        t = jnp.where(t >= rows, t - rows, t)
    pos = z * rows + t
    j = lax.broadcasted_iota(jnp.int32, (HALF, cols), 0)
    on_row = j < QUARTER
    freq = jnp.exp(jnp.where(on_row, j, j - QUARTER).astype(jnp.float32) * (-math.log(theta_base) / QUARTER))
    angle = jnp.where(on_row, pos // GRID_W, lax.rem(pos, GRID_W)).astype(jnp.float32) * freq
    tab[0] = jnp.cos(angle)
    tab[1] = jnp.sin(angle)
    diag = lax.broadcasted_iota(jnp.int32, (HEAD_DIM, HEAD_DIM), 0) == lax.broadcasted_iota(
        jnp.int32, (HEAD_DIM, HEAD_DIM), 1
    )

    def column(ref):
        return jnp.sum(jnp.where(diag, ref[...], 0.0), axis=1, keepdims=True)

    vt[:, HEAD_DIM:, :] = jnp.ones((KV_HEADS, ONES, vt.shape[2]), jnp.bfloat16)
    qbd[...] = jnp.zeros(qbd.shape, jnp.bfloat16)
    acc[...] = jnp.zeros(acc.shape, jnp.float32)
    top[...] = jnp.full(top.shape, -1e30, jnp.float32)

    pl.semaphore_wait(barrier, 5)

    def piece(cls, xi, p):
        if cls == 0:
            return (wk, wv)[p].at[xi, c]
        return (wq, wo)[cls - 1].at[xi, c, p]

    def lane(cls, p):
        return cls + 1 if cls else p

    def ring_copy(cls, d, s, p):
        owner = lax.rem(x + (nx - s + 1 if d == 0 else s - 1), nx)
        ref = piece(cls, owner, p)
        return pltpu.make_async_remote_copy(
            src_ref=ref, dst_ref=ref, send_sem=ring_send.at[cls],
            recv_sem=ring_recv.at[cls, d, s - 1, p],
            device_id=to_x[d], device_id_type=MESH,
        )

    def core_copy(cls, xi, p):
        ref = piece(cls, xi, p)
        pltpu.make_async_remote_copy(
            src_ref=ref, dst_ref=ref, send_sem=d2d_send.at[lane(cls, p)],
            recv_sem=d2d_recv.at[lane(cls, p)],
            device_id=to_core, device_id_type=MESH,
        ).start()

    def start_own(cls):
        for p in range(2):
            for d in range(2):
                ring_copy(cls, d, 1, p).start()
        for p in range(2):
            core_copy(cls, x, p)

    def arrive_w(cls, d, s, p):
        owner = lax.rem(x + (nx - s if d == 0 else s), nx)
        ref = piece(cls, owner, p)
        pltpu.make_async_copy(ref, ref, ring_recv.at[cls, d, s - 1, p]).wait()
        if s + 1 < h_x or (s + 1 == h_x and p == d):
            ring_copy(cls, d, s + 1, p).start()
        core_copy(cls, owner, p)

    def z_slot(d, s):
        return 0 if s == 0 else (2 * s - 1 if d == 0 or s == h_z else 2 * s)

    def z_send_piece(d, s, p):
        buf = (kbuf, vbuf)[p]
        pltpu.make_async_remote_copy(
            src_ref=buf.at[z_slot(d, s - 1)], dst_ref=buf.at[z_slot(d, s)],
            send_sem=z_send.at[p], recv_sem=z_recv.at[d, s - 1, p],
            device_id=to_z[d], device_id_type=MESH,
        ).start()

    def arrive_z(d, s, p):
        ref = (kbuf, vbuf)[p].at[z_slot(d, s)]
        pltpu.make_async_copy(ref, ref, z_recv.at[d, s - 1, p]).wait()
        if s + 1 < h_z or (s + 1 == h_z and p == d):
            z_send_piece(d, s + 1, p)

    def core_wait(i):
        ref = (wk.at[:, other], wv.at[:, other], wq.at[:, other], wo.at[:, other])[i]
        pltpu.make_async_copy(ref, ref, d2d_recv.at[i]).wait()

    def project(weight):
        total = jnp.zeros((rows, weight.shape[-1]), jnp.float32)
        for i in range(nx):
            total += jnp.dot(
                tok[:, 2 * wrows * i:2 * wrows * (i + 1)],
                weight[i].reshape(2 * wrows, weight.shape[-1]),
                preferred_element_type=jnp.float32,
            )
        return total

    def make_kv():
        core_wait(1)
        vbuf[0] = project(wv).astype(jnp.bfloat16)
        core_wait(0)
        raw = project(wk)
        width = KV_HEADS * HEAD_DIM
        padded = jnp.concatenate([raw, jnp.zeros((width - rows, width), jnp.float32)], axis=0).T
        gain = column(kg_in)
        cosine, sine = tab[0, :, :width], tab[1, :, :width]
        turned = jnp.concatenate(
            [
                norm_rotate_t(padded[HEAD_DIM * i:HEAD_DIM * (i + 1)], gain, cosine, sine)
                for i in range(KV_HEADS)
            ],
            axis=0,
        ).T
        kbuf[0] = turned[:rows].astype(jnp.bfloat16)
        for p in (1, 0):
            for d in range(2):
                z_send_piece(d, 1, p)

    def make_q():
        core_wait(2)
        tile = 256

        @pl.loop(0, HEADS * HEAD_DIM // tile)
        def _(n):
            at = pl.ds(pl.multiple_of(n * tile, tile), tile)
            total = jnp.zeros((rows, tile), jnp.float32)
            for i in range(nx):
                total += jnp.dot(
                    tok[:, 2 * wrows * i:2 * wrows * (i + 1)],
                    wq[i, :, :, :, at].reshape(2 * wrows, tile),
                    preferred_element_type=jnp.float32,
                )
            rawq[:, at] = total

        gain = column(qg_in)
        for g in range(KV_HEADS):
            both = jnp.concatenate(
                [rawq[:, 256 * g:256 * g + 128], rawq[:, 256 * g + 128:256 * g + 256]], axis=0
            )
            stacked = jnp.concatenate([both, pltpu.roll(both, 64, 1)], axis=0)
            raw = stacked.T[:HEAD_DIM]
            at = (g % 2) * HEAD_DIM
            qbd[g, at:at + HEAD_DIM, :] = norm_rotate_t(raw, gain, tab[0], tab[1]).astype(jnp.bfloat16)

    factor = HEAD_DIM ** (-0.5) * math.log2(math.e)
    edges = list(range(0, cols, 256)) + [cols]

    def attend(u):
        keys = 2 * rows
        v = vbuf[2 * u:2 * u + 2].reshape(keys, KV_HEADS * HEAD_DIM).astype(jnp.float32)
        v = jnp.concatenate([v, jnp.zeros((vt.shape[2] - keys, v.shape[1]), jnp.float32)], axis=0)
        v = v.T.astype(jnp.bfloat16)
        for g in range(KV_HEADS):
            vt[g, :HEAD_DIM, :] = v[HEAD_DIM * g:HEAD_DIM * (g + 1)]

        @pl.loop(0, KV_HEADS)
        def _(g):
            block = pl.ds(pl.multiple_of((g // 2) * 128, 128), 128)
            k = kbuf[2 * u:2 * u + 2, :, block].reshape(keys, 128)
            for a, b in zip(edges[:-1], edges[1:]):
                s = jnp.dot(k, qbd[g, :, a:b], preferred_element_type=jnp.float32) * factor
                old = top[g, :, a:b]
                new = jnp.maximum(old, jnp.max(s, axis=0, keepdims=True))
                p = jnp.exp2(s - new).astype(jnp.bfloat16)
                o = jnp.dot(vt[g, :, :keys], p, preferred_element_type=jnp.float32)
                acc[g, :, a:b] = acc[g, :, a:b] * jnp.exp2(old - new) + o
                top[g, :, a:b] = new

    def finish():
        for g in range(KV_HEADS):
            o = acc[g, :HEAD_DIM] / acc[g, HEAD_DIM:HEAD_DIM + 1]
            o = jnp.concatenate([o, jnp.zeros((128 - HEAD_DIM, cols), jnp.float32)], axis=0).T
            y = (o[:2 * rows] + pltpu.roll(o[2 * rows:], 64, 1)).astype(jnp.bfloat16)
            att[:, 256 * g:256 * g + 128] = y[:rows]
            att[:, 256 * g + 128:256 * g + 256] = y[rows:]

    def project_out():
        core_wait(3)
        depth = att.shape[1]
        width = 2 * wo.shape[-1]

        @pl.loop(0, nx)
        def _(i):
            w = jnp.concatenate(
                [wo[i, 0].reshape(depth, width // 2), wo[i, 1].reshape(depth, width // 2)], axis=1
            )
            out_ref[0, :, pl.ds(pl.multiple_of(i * width, width), width)] = jnp.dot(
                att[...], w, preferred_element_type=jnp.float32
            ).astype(jnp.bfloat16)

    loads[0].wait()
    loads[1].wait()
    start_own(0)
    for cp in loads[2:]:
        cp.wait()

    left = {0: 0, 1: 0, 2: 0}
    events = make_schedule(nx, nz)
    last_forward = {}
    for e in events:
        if e[1] == "w":
            left[e[2]] += 1
            if e[4] < h_x:
                last_forward[e[2]] = e
    seen_z = {}
    done_units, q_ready, clock = 0, False, 0.0

    def arrived_units():
        n = 0
        while n < h_z:
            need = [(d, s, p) for s in range(1, n + 2) for d in range(2) for p in range(2)
                    if z_slot(d, s) <= 2 * n + 1 and not (s == h_z and p != d)]
            if all(k in seen_z for k in need):
                n += 1
            else:
                break
        return n

    for e in events:
        clock = max(clock, e[0])
        if q_ready and done_units < arrived_units():
            while done_units < arrived_units() and clock + UNIT_US * 0.5 <= e[0] + 0.01 + UNIT_US:
                attend(done_units)
                done_units += 1
                clock += UNIT_US
                break
        if e[1] == "w":
            _, _, cls, d, s, p = e
            arrive_w(cls, d, s, p)
            left[cls] -= 1
            if cls < 2 and e is last_forward[cls]:
                start_own(cls + 1)
            if left[cls] == 0 and cls == 0:
                make_kv()
            if left[cls] == 0 and cls == 1:
                make_q()
                q_ready = True
        else:
            _, _, d, s, p = e
            arrive_z(d, s, p)
            seen_z[(d, s, p)] = True
    while done_units < h_z:
        attend(done_units)
        done_units += 1
    finish()
    project_out()

    def drain(ref, sem):
        pltpu.make_async_copy(ref, ref, sem).wait()

    drain(wk.at[0:nx - 1], ring_send.at[0])
    drain(wq.at[0:nx - 1, 0], ring_send.at[1])
    drain(wo.at[0:nx - 1, 0], ring_send.at[2])
    for i, ref in enumerate((wk, wv, wq, wo)):
        drain(ref.at[:, c], d2d_send.at[i])
    drain(kbuf.at[0:nz - 1], z_send.at[0])
    drain(vbuf.at[0:nz - 1], z_send.at[1])


def shards(nx, nz, tokens, query_weight, key_weight, value_weight, out_weight, query_gain, key_gain):
    rows, width = tokens.shape[1], tokens.shape[2]
    wrows, qcols = query_weight.shape
    kcols = key_weight.shape[1]
    odepth, ocols = out_weight.shape
    cols = PER_KV * rows
    keys = -(-2 * rows // 128) * 128
    bf, f32 = jnp.bfloat16, jnp.float32
    dma = pltpu.SemaphoreType.DMA
    anywhere = pl.BlockSpec(memory_space=pl.ANY)
    vmem = pl.BlockSpec(memory_space=pltpu.VMEM)
    return pl.pallas_call(
        lambda *refs: kernel(nx, nz, *refs),
        out_shape=jax.ShapeDtypeStruct(tokens.shape[:2] + (2 * nx * ocols,), bf),
        in_specs=[anywhere] * 5 + [vmem] * 2,
        out_specs=vmem,
        scratch_shapes=[
            pltpu.VMEM((rows, width), bf),
            pltpu.VMEM((nx, 2, 2, wrows // 2, qcols), bf),
            pltpu.VMEM((nx, 2, wrows, kcols), bf),
            pltpu.VMEM((nx, 2, wrows, kcols), bf),
            pltpu.VMEM((nx, 2, 2, odepth // 2, ocols), bf),
            pltpu.VMEM((nz, rows, kcols), bf),
            pltpu.VMEM((nz, rows, kcols), bf),
            pltpu.VMEM((KV_HEADS, VROWS, keys), bf),
            pltpu.VMEM((KV_HEADS, 2 * HEAD_DIM, cols), bf),
            pltpu.VMEM((rows, qcols), f32),
            pltpu.VMEM((2, HALF, cols), f32),
            pltpu.VMEM((KV_HEADS, VROWS, cols), f32),
            pltpu.VMEM((KV_HEADS, 1, cols), f32),
            pltpu.VMEM((rows, qcols), bf),
            dma((3, 2, nx // 2, 2)),
            dma((3,)),
            dma((4,)),
            dma((4,)),
            dma((2, nz // 2, 2)),
            dma((2,)),
            dma((7,)),
        ],
        compiler_params=pltpu.CompilerParams(
            collective_id=0, has_side_effects=True, vmem_limit_bytes=50 * 1024 * 1024
        ),
    )(tokens, query_weight, key_weight, value_weight, out_weight,
      query_gain.reshape(1, -1), key_gain.reshape(1, -1))


def solution(mesh):
    nx, nz = mesh.shape["dp"] // 2, mesh.shape["sp"]
    in_specs = (
        P(("grp", "dp"), "sp", None),
        P("dp", None),
        P("dp", None),
        P("dp", None),
        P(None, "dp"),
        P(),
        P(),
    )
    out_specs = P(("grp", "dp"), "sp", None)

    def body(*args):
        return shards(nx, nz, *args)

    return jax.shard_map(body, mesh=mesh, in_specs=in_specs, out_specs=out_specs, check_vma=False)
```

```python
import math

import jax
import jax.numpy as jnp
from jax import lax
from jax.experimental import pallas as pl
from jax.experimental.pallas import tpu as pltpu
from jax.sharding import PartitionSpec as P

HEADS = 16
KV_HEADS = 4
HEAD_DIM = 64
GRID_W = 64
PER_KV = HEADS // KV_HEADS
HALF = HEAD_DIM // 2
QUARTER = HEAD_DIM // 4

theta_base = 10000.0
norm_eps = 1e-06
MESH = pl.DeviceIdType.MESH
LIMIT = 63 * 1024 * 1024
ONES = 16
VROWS = HEAD_DIM + ONES

PARTS = (
    None,
    (("all", 1 / 4), ("all", 1 / 4), ("own", 1 / 4)),
    (("all", 1 / 4), ("own", 3 / 16), ("own", 3 / 16)),
)

KV_AT, KV_STEP, KV_CUT = 2.8, 3.2, 0.7
Q_AT, Q_STEP, Q_CUT = 15.0, 4.2, 1.4
O_AT, O_STEP, O_CUT = 30.0, 3.6, 1.2
Y_LATE = 4.0
Z_AT, Z_STEP, Z_CUT = 19.0, 3.5, 0.85
X_MARGIN, Z_EARLY = 0.2, 0.2
KV_US, Q_US, UNIT_US = 1.5, 0.7, 0.4


def norm_rotate_t(raw, gain, cosine, sine):
    inv = lax.rsqrt(jnp.mean(raw * raw, axis=0, keepdims=True) + norm_eps)
    scaled = raw * inv * gain
    first, second = scaled[:HALF], scaled[HALF:]
    return jnp.concatenate(
        [first * cosine - second * sine, second * cosine + first * sine], axis=0
    )


def n_pieces(cls):
    return 4 if cls == 0 else len(PARTS[cls])


def far_way(cls, p):
    return int(p >= 2) if cls == 0 else int(p >= 1)


def make_schedule(nx, nz):
    h, hz = nx // 2, nz // 2
    xy, along_z = [], []
    timing = ((KV_AT, KV_STEP, KV_CUT), (Q_AT, Q_STEP, Q_CUT), (O_AT, O_STEP, O_CUT))
    for cls, (first, step, gap) in enumerate(timing):
        for s in range(1, h + 1):
            for d in range(2):
                count = 0
                for p in range(n_pieces(cls)):
                    if s == h and far_way(cls, p) != d:
                        continue
                    at = first + (s - 1) * step + gap * count
                    count += 1
                    xy.append((at, "w", cls, d, s, p))
                    if cls and PARTS[cls][p][0] == "own":
                        xy.append((at + Y_LATE, "y", cls, d, s, p))
    for s in range(1, hz + 1):
        for d in range(2):
            count = 0
            for p in range(4):
                if s == hz and far_way(0, p) != d:
                    continue
                along_z.append((Z_AT + (s - 1) * Z_STEP + Z_CUT * count, "z", d, s, p))
                count += 1
    return sorted(xy, key=lambda e: e[0]), sorted(along_z, key=lambda e: e[0])


def kernel(nx, nz, tok_in, wq_in, wk_in, wv_in, wo_in, qg_in, kg_in, out_ref,
           tok, wq, wk, wv, wo, kbuf, vbuf, vt, qbd, tab, acc, top, sbuf, pbuf, fade, att,
           ring_recv, ring_send, d2d_recv, d2d_send, z_recv, z_send, y_recv, y_send, loc):
    h_x, h_z = nx // 2, nz // 2
    rows = tok.shape[0]
    cols = PER_KV * rows
    dp = lax.axis_index("dp")
    z = lax.axis_index("sp")
    x, c = dp // 2, lax.rem(dp, 2)
    other = 1 - c
    to_x = ({"dp": lax.rem(dp + 2, 2 * nx)}, {"dp": lax.rem(dp + 2 * nx - 2, 2 * nx)})
    to_z = ({"sp": lax.rem(z + 1, nz)}, {"sp": lax.rem(z + nz - 1, nz)})
    to_core = {"dp": 2 * x + other}
    grp = lax.axis_index("grp")
    share = lax.rem(grp, 2)
    to_pair = {"grp": grp + 1 - 2 * share}

    wrows = wk.shape[2]
    loads = []

    def load(src, dst):
        cp = pltpu.make_async_copy(src, dst, loc.at[len(loads)])
        cp.start()
        loads.append(cp)

    load(wk_in, wk.at[x, c])
    load(wv_in, wv.at[x, c])
    load(tok_in.at[0], tok)
    load(wq_in, wq.at[x, c])
    load(wo_in, wo.at[x, c])

    barrier = pltpu.get_barrier_semaphore()
    for peer in (*to_x, *to_z, to_core, to_pair):
        pl.semaphore_signal(barrier, inc=1, device_id=peer, device_id_type=MESH)

    t = lax.broadcasted_iota(jnp.int32, (HALF, cols), 1)
    for _ in range(PER_KV - 1):
        t = jnp.where(t >= rows, t - rows, t)
    pos = z * rows + t
    j = lax.broadcasted_iota(jnp.int32, (HALF, cols), 0)
    on_row = j < QUARTER
    freq = jnp.exp(jnp.where(on_row, j, j - QUARTER).astype(jnp.float32) * (-math.log(theta_base) / QUARTER))
    angle = jnp.where(on_row, pos // GRID_W, lax.rem(pos, GRID_W)).astype(jnp.float32) * freq
    tab[0] = jnp.cos(angle)
    tab[1] = jnp.sin(angle)
    diag = lax.broadcasted_iota(jnp.int32, (HEAD_DIM, HEAD_DIM), 0) == lax.broadcasted_iota(
        jnp.int32, (HEAD_DIM, HEAD_DIM), 1
    )

    def column(ref):
        return jnp.sum(jnp.where(diag, ref[...], 0.0), axis=1, keepdims=True)

    vt[:, :, HEAD_DIM:, :] = jnp.ones((2, KV_HEADS, ONES, vt.shape[3]), jnp.bfloat16)
    qbd[...] = jnp.zeros(qbd.shape, jnp.bfloat16)
    acc[...] = jnp.zeros(acc.shape, jnp.float32)
    top[...] = jnp.full(top.shape, -1e30, jnp.float32)

    with jax.named_scope('barrier'):
        pl.semaphore_wait(barrier, 6)

    def cut(cls, p, theirs=False):
        total = (wq, wo)[cls - 1].shape[2]
        sizes = [int(total * f) for _, f in PARTS[cls]]
        kinds = [k for k, _ in PARTS[cls]]
        start, size = sum(sizes[:p]), sizes[p]
        if kinds[p] == "all":
            return start, size
        own = sum(n for n, k in zip(sizes, kinds) if k == "own")
        return pl.multiple_of(start + own * (1 - share if theirs else share), 16), size

    def piece(cls, xi, p, theirs=False):
        if cls == 0:
            return (wk, wv)[p % 2].at[xi, c, pl.ds((p // 2) * (wrows // 2), wrows // 2)]
        start, size = cut(cls, p, theirs)
        return (wq, wo)[cls - 1].at[xi, c, pl.ds(start, size)]

    def lane(cls, p):
        return cls + 1 if cls else p % 2

    def ring_copy(cls, d, s, p):
        owner = lax.rem(x + (nx - s + 1 if d == 0 else s - 1), nx)
        ref = piece(cls, owner, p)
        return pltpu.make_async_remote_copy(
            src_ref=ref, dst_ref=ref, send_sem=ring_send.at[cls],
            recv_sem=ring_recv.at[cls, d, s - 1, p],
            device_id=to_x[d], device_id_type=MESH,
        )

    def core_copy(lane_id, ref):
        pltpu.make_async_remote_copy(
            src_ref=ref, dst_ref=ref, send_sem=d2d_send.at[lane_id], recv_sem=d2d_recv.at[lane_id],
            device_id=to_core, device_id_type=MESH,
        ).start()

    def start_own(cls):
        for p in range(n_pieces(cls)):
            for d in range(2):
                ring_copy(cls, d, 1, p).start()
        if cls == 0:
            core_copy(0, wk.at[x, c])
            core_copy(1, wv.at[x, c])
        else:
            core_copy(cls + 1, (wq, wo)[cls - 1].at[x, c])

    def owner_of(d, s):
        return lax.rem(x + (nx - s if d == 0 else s), nx)

    def arrive_y(cls, d, s, p):
        ref = piece(cls, owner_of(d, s), p, theirs=True)
        pltpu.make_async_copy(ref, ref, y_recv.at[cls - 1, d, s - 1, p]).wait()
        core_copy(lane(cls, p), ref)

    def arrive_w(cls, d, s, p):
        ref = piece(cls, owner_of(d, s), p)
        pltpu.make_async_copy(ref, ref, ring_recv.at[cls, d, s - 1, p]).wait()
        if s + 1 < h_x or (s + 1 == h_x and far_way(cls, p) == d):
            ring_copy(cls, d, s + 1, p).start()
        if cls and PARTS[cls][p][0] == "own":
            pltpu.make_async_remote_copy(
                src_ref=ref, dst_ref=ref, send_sem=y_send.at[cls - 1],
                recv_sem=y_recv.at[cls - 1, d, s - 1, p],
                device_id=to_pair, device_id_type=MESH,
            ).start()
        core_copy(lane(cls, p), ref)

    def z_slot(d, s):
        return 0 if s == 0 else (2 * s - 1 if d == 0 or s == h_z else 2 * s)

    def z_piece(slot, p):
        return (vbuf, kbuf)[p // 2].at[slot, pl.ds((p % 2) * (rows // 2), rows // 2)]

    def z_send_piece(d, s, p):
        pltpu.make_async_remote_copy(
            src_ref=z_piece(z_slot(d, s - 1), p), dst_ref=z_piece(z_slot(d, s), p),
            send_sem=z_send.at[p // 2], recv_sem=z_recv.at[d, s - 1, p],
            device_id=to_z[d], device_id_type=MESH,
        ).start()

    def arrive_z(d, s, p):
        ref = z_piece(z_slot(d, s), p)
        pltpu.make_async_copy(ref, ref, z_recv.at[d, s - 1, p]).wait()
        if s + 1 < h_z or (s + 1 == h_z and far_way(0, p) == d):
            z_send_piece(d, s + 1, p)

    def core_wait(i):
        ref = (wk.at[:, other], wv.at[:, other], wq.at[:, other], wo.at[:, other])[i]
        pltpu.make_async_copy(ref, ref, d2d_recv.at[i]).wait()

    def project(weight):
        total = jnp.zeros((rows, weight.shape[-1]), jnp.float32)
        for i in range(nx):
            total += jnp.dot(
                tok[:, 2 * wrows * i:2 * wrows * (i + 1)],
                weight[i].reshape(2 * wrows, weight.shape[-1]),
                preferred_element_type=jnp.float32,
            )
        return total

    def make_kv():
        core_wait(1)
        vbuf[0] = project(wv).astype(jnp.bfloat16)
        core_wait(0)
        raw = project(wk)
        width = KV_HEADS * HEAD_DIM
        padded = jnp.concatenate([raw, jnp.zeros((width - rows, width), jnp.float32)], axis=0).T
        gain = column(kg_in)
        cosine, sine = tab[0, :, :width], tab[1, :, :width]
        turned = jnp.concatenate(
            [
                norm_rotate_t(padded[HEAD_DIM * i:HEAD_DIM * (i + 1)], gain, cosine, sine)
                for i in range(KV_HEADS)
            ],
            axis=0,
        ).T
        kbuf[0] = turned[:rows].astype(jnp.bfloat16)
        for p in range(4):
            for d in range(2):
                z_send_piece(d, 1, p)

    def make_q(g):
        at = slice(2 * 128 * g, 2 * 128 * (g + 1))
        total = jnp.zeros((rows, 256), jnp.float32)
        for i in range(nx):
            total += jnp.dot(
                tok[:, 2 * wrows * i:2 * wrows * (i + 1)],
                wq[i, :, :, at].reshape(2 * wrows, 256),
                preferred_element_type=jnp.float32,
            )
        both = jnp.concatenate([total[:, :128], total[:, 128:]], axis=0)
        stacked = jnp.concatenate([both, pltpu.roll(both, 64, 1)], axis=0)
        raw = stacked.T[:HEAD_DIM]
        at = (g % 2) * HEAD_DIM
        turned = norm_rotate_t(raw, column(qg_in), tab[0], tab[1])
        qbd[g, at:at + HEAD_DIM, :] = turned.astype(jnp.bfloat16)

    factor = HEAD_DIM ** (-0.5) * math.log2(math.e)
    edges = list(range(0, cols, 256)) + [cols]

    keys = 2 * rows

    def load_v(u):
        v = vbuf[2 * u:2 * u + 2].reshape(keys, KV_HEADS * HEAD_DIM).astype(jnp.float32)
        v = jnp.concatenate([v, jnp.zeros((vt.shape[3] - keys, v.shape[1]), jnp.float32)], axis=0)
        v = v.T.astype(jnp.bfloat16)
        for g in range(KV_HEADS):
            vt[u % 2, g, :HEAD_DIM, :] = v[HEAD_DIM * g:HEAD_DIM * (g + 1)]

    def attend(n):
        last = h_z * KV_HEADS
        for a, b in zip(edges[:-1], edges[1:]):
            if n >= 2:
                u, g = divmod(n - 2, KV_HEADS)
                o = jnp.dot(vt[u % 2, g, :, :keys], pbuf[n % 2, :, a:b], preferred_element_type=jnp.float32)
                acc[g, :, a:b] = acc[g, :, a:b] * fade[n % 2, :, a:b] + o
            if 1 <= n <= last:
                g = (n - 1) % KV_HEADS
                s = sbuf[(n - 1) % 2, :, a:b]
                pbuf[(n - 1) % 2, :, a:b] = jnp.exp2(s * factor - top[g, :, a:b]).astype(jnp.bfloat16)
            if n < last:
                u, g = divmod(n, KV_HEADS)
                at = (g // 2) * 128
                k = kbuf[2 * u:2 * u + 2, :, at:at + 128].reshape(keys, 128)
                s = jnp.dot(k, qbd[g, :, a:b], preferred_element_type=jnp.float32)
                old = top[g, :, a:b]
                new = jnp.maximum(old, jnp.max(s, axis=0, keepdims=True) * factor)
                sbuf[n % 2, :, a:b] = s
                fade[n % 2, :, a:b] = jnp.exp2(old - new)
                top[g, :, a:b] = new

    def finish():
        for g in range(KV_HEADS):
            o = acc[g, :HEAD_DIM] / acc[g, HEAD_DIM:HEAD_DIM + 1]
            o = jnp.concatenate([o, jnp.zeros((128 - HEAD_DIM, cols), jnp.float32)], axis=0).T
            y = (o[:2 * rows] + pltpu.roll(o[2 * rows:], 64, 1)).astype(jnp.bfloat16)
            att[:, 256 * g:256 * g + 128] = y[:rows]
            att[:, 256 * g + 128:256 * g + 256] = y[rows:]

    def project_out():
        core_wait(3)
        width = 2 * wo.shape[-1]

        for i in range(nx):
            w = jnp.concatenate([wo[i, 0], wo[i, 1]], axis=1)
            out_ref[0, :, i * width:(i + 1) * width] = jnp.dot(
                att[...], w, preferred_element_type=jnp.float32
            ).astype(jnp.bfloat16)

    with jax.named_scope('loads'):
        loads[0].wait()
        loads[1].wait()
    start_own(0)
    for cp in loads[2:]:
        cp.wait()

    xy, along_z = make_schedule(nx, nz)
    left = [sum(e[2] == cls for e in xy) for cls in range(3)]
    forwards = [sum(e[1] == "w" and e[2] == cls and e[4] < h_x for e in xy) for cls in range(3)]
    seen, clock = set(), 0.0
    q_work, steps, all_steps = [], 0, h_z * KV_HEADS + 2

    def unit_ready(u):
        return all(
            ("z", d, s, p) in seen
            for s in range(1, h_z + 1) for d in range(2) for p in range(4)
            if z_slot(d, s) // 2 == u and (s < h_z or far_way(0, p) == d)
        )

    def do_xy(e):
        _, kind, cls, d, s, p = e
        with jax.named_scope(f'{kind}{cls}{d}{s}{p}'):
            (arrive_w if kind == "w" else arrive_y)(cls, d, s, p)
        left[cls] -= 1
        if kind == "w" and s < h_x:
            forwards[cls] -= 1
            if forwards[cls] == 0 and cls < 2:
                start_own(cls + 1)
        if left[cls] == 0 and cls == 0:
            with jax.named_scope('make_kv'):
                make_kv()
            return KV_US
        if left[cls] == 0 and cls == 1:
            q_work.extend(range(KV_HEADS + 1))
        return 0.03

    def next_work():
        nonlocal steps
        if q_work:
            g = q_work.pop(0)
            with jax.named_scope(f'q{g}'):
                if g == 0:
                    core_wait(2)
                else:
                    make_q(g - 1)
            return Q_US if g else 0.05
        n, steps = steps, steps + 1
        u, g = divmod(n, KV_HEADS)
        with jax.named_scope(f'a{u}{g}'):
            if g == 0 and u < h_z:
                load_v(u)
            attend(n)
        return UNIT_US

    def has_work():
        if q_work:
            return True
        u = steps // KV_HEADS
        return left[1] == 0 and steps < all_steps and (u >= h_z or unit_ready(u))

    while xy or along_z or has_work():
        if along_z and left[0] == 0 and along_z[0][0] <= clock + Z_EARLY:
            e = along_z.pop(0)
        elif xy and xy[0][0] + X_MARGIN <= clock:
            e = xy.pop(0)
        elif has_work():
            clock += next_work()
            continue
        elif along_z and left[0] == 0 and (not xy or along_z[0][0] < xy[0][0] + X_MARGIN):
            e = along_z.pop(0)
        else:
            e = xy.pop(0)
        clock = max(clock, e[0])
        if e[1] == "z":
            with jax.named_scope(f'z{e[2]}{e[3]}{e[4]}'):
                arrive_z(*e[2:])
            seen.add(e[1:])
        else:
            clock += do_xy(e)
    with jax.named_scope('finish'):
        finish()
    with jax.named_scope('out'):
        project_out()

    def drain(ref, sem):
        pltpu.make_async_copy(ref, ref, sem).wait()

    drain(wk.at[0:nx - 1], ring_send.at[0])
    for i, w in enumerate((wq, wo)):
        sent = sum(cut(i + 1, p)[1] for p in range(n_pieces(i + 1)))
        part = sum(cut(i + 1, p)[1] for p, (k, _) in enumerate(PARTS[i + 1]) if k == "own")
        drain(w.at[0:nx - 1, 0, 0:sent], ring_send.at[i + 1])
        drain(w.at[0:nx - 1, 0, 0:part], y_send.at[i])
    for i, ref in enumerate((wk, wv, wq, wo)):
        drain(ref.at[:, c], d2d_send.at[i])
    drain(vbuf.at[0:nz - 1], z_send.at[0])
    drain(kbuf.at[0:nz - 1], z_send.at[1])


def shards(nx, nz, tokens, query_weight, key_weight, value_weight, out_weight, query_gain, key_gain):
    rows, width = tokens.shape[1], tokens.shape[2]
    wrows, qcols = query_weight.shape
    kcols = key_weight.shape[1]
    odepth, ocols = out_weight.shape
    cols = PER_KV * rows
    keys = -(-2 * rows // 128) * 128
    bf, f32 = jnp.bfloat16, jnp.float32
    dma = pltpu.SemaphoreType.DMA
    hbm = pl.BlockSpec(memory_space=pltpu.HBM)
    vmem = pl.BlockSpec(memory_space=pltpu.VMEM)
    return pl.pallas_call(
        lambda *refs: kernel(nx, nz, *refs),
        out_shape=jax.ShapeDtypeStruct(tokens.shape[:2] + (2 * nx * ocols,), bf),
        in_specs=[hbm] * 5 + [vmem] * 2,
        out_specs=vmem,
        scratch_shapes=[
            pltpu.VMEM((rows, width), bf),
            pltpu.VMEM((nx, 2, wrows, qcols), bf),
            pltpu.VMEM((nx, 2, wrows, kcols), bf),
            pltpu.VMEM((nx, 2, wrows, kcols), bf),
            pltpu.VMEM((nx, 2, odepth, ocols), bf),
            pltpu.VMEM((nz, rows, kcols), bf),
            pltpu.VMEM((nz, rows, kcols), bf),
            pltpu.VMEM((2, KV_HEADS, VROWS, keys), bf),
            pltpu.VMEM((KV_HEADS, 2 * HEAD_DIM, cols), bf),
            pltpu.VMEM((2, HALF, cols), f32),
            pltpu.VMEM((KV_HEADS, VROWS, cols), f32),
            pltpu.VMEM((KV_HEADS, 1, cols), f32),
            pltpu.VMEM((2, 2 * rows, cols), f32),
            pltpu.VMEM((2, 2 * rows, cols), bf),
            pltpu.VMEM((2, 1, cols), f32),
            pltpu.VMEM((rows, qcols), bf),
            dma((3, 2, nx // 2, 4)),
            dma((3,)),
            dma((4,)),
            dma((4,)),
            dma((2, nz // 2, 4)),
            dma((2,)),
            dma((2, 2, nx // 2, 3)),
            dma((2,)),
            dma((5,)),
        ],
        compiler_params=pltpu.CompilerParams(
            collective_id=0, has_side_effects=True, vmem_limit_bytes=LIMIT
        ),
    )(tokens, query_weight, key_weight, value_weight, out_weight,
      query_gain.reshape(1, -1), key_gain.reshape(1, -1))


def solution(mesh):
    nx, nz = mesh.shape["dp"] // 2, mesh.shape["sp"]
    in_specs = (
        P(("grp", "dp"), "sp", None),
        P("dp", None),
        P("dp", None),
        P("dp", None),
        P(None, "dp"),
        P(),
        P(),
    )
    out_specs = P(("grp", "dp"), "sp", None)

    def body(*args):
        return shards(nx, nz, *args)

    return jax.shard_map(body, mesh=mesh, in_specs=in_specs, out_specs=out_specs, check_vma=False)
```
